256 devices in a mesh: grp: 2 (over y), sp: 32 (over z, core), tp: 4 (over x).
Axes of the slice: x: 4, y: 2, z: 16, core: 2. Of those that a mesh axis runs over, the one named last changes fastest.
The devices are a block of a 4x16x16 slice.
Arguments:
- tokens: bfloat16 [196608, 2048], P(('grp', 'sp', 'tp')), parts along dimension 0, may hold values from -6 to 6
- gain_pre: float32 [2, 2048], replicated, may hold values from 0.1 to 1.9
- gain_post: float32 [2, 2048], replicated, may hold values from 0.1 to 1.9
- w_b: bfloat16 [2, 2048, 512], P(None, 'sp', 'tp'), may hold values from -0.125 to 0.125
- w_c: bfloat16 [2, 2048, 512], P(None, 'sp', 'tp'), may hold values from -0.125 to 0.125
- w_x: bfloat16 [2, 2048, 512], P(None, 'sp', 'tp'), may hold values from -0.125 to 0.125
- taps: float32 [2, 3, 512], replicated, may hold values from -3.5 to 3.5
- w_out: bfloat16 [2, 512, 2048], P(None, 'tp', 'sp'), may hold values from -0.25 to 0.25
Outputs:
- result: bfloat16 [196608, 2048], P(('grp', 'sp', 'tp')), parts along dimension 0
The draws below stay inside these ranges and needn't reach their ends.
There are 2 independent parts, one for each index of `grp`. The reference program is written for one: setup_inputs(seed, part) draws one part's arguments, and reference() takes and returns one part's arrays. A program takes and returns all parts, laid end to end along the dimension named above; an argument that names none is the same for every part. Nothing has to cross between parts.
All inputs are finite; a program needn't handle non-finite values.
Results may differ from the reference program's by a relative error of at most 0.024.
Values may be sent and summed in bfloat16 or wider, within the bound.
No kernel may reach another device: no remote copies, remote signals or barrier semaphores. Data moves between devices by JAX's collectives and lax.ppermute only.
A program may use at most 128 MiB of HBM per device.

```python
import jax
import jax.numpy as jnp
from jax import lax

D = 2048
DC = 512
KERNEL = 3
LAYERS = 2
TOKENS = 98304


def level_of(own_key, dims, cuts, least, high):
    def one(dim, parts):
        draws = jax.random.uniform(jax.random.fold_in(jax.random.fold_in(own_key, 6), dim), (parts,), jnp.float32, least / len(cuts), high / len(cuts))
        return jnp.repeat(jnp.exp(draws), dims[dim] // parts).reshape((-1,) + (1,) * (len(dims) - dim - 1))

    gain = one(*cuts[0])
    for cut in cuts[1:]:
        gain = gain * one(*cut)
    return gain


def centred(stream_key, extent, scale, reach, cuts=(), held_as=jnp.bfloat16):
    result = jax.random.normal(stream_key, extent, jnp.float32) * scale
    if len(cuts) > 0:
        result = level_of(stream_key, extent, cuts, -0.22, 0.18) * result
    return jnp.clip(result, min=-reach, max=reach).astype(held_as)


def setup_inputs(seed: int = 0, part: int = 0) -> dict:
    key_of = jax.random.split(jax.random.key(seed), 9)
    part_splits = jax.random.split(jax.random.fold_in(key_of[8], part), 9)
    return {
        "tokens": centred(part_splits[0], (TOKENS, D), 1.0, 6.0, ((0, 128),)),
        "gain_pre": jnp.clip(1.0 + 0.18 * jax.random.normal(key_of[1], (LAYERS, D), jnp.float32), 0.1, 1.9),
        "gain_post": jnp.clip(1.0 + 0.18 * jax.random.normal(key_of[2], (LAYERS, D), jnp.float32), 0.1, 1.9),
        "w_b": centred(key_of[3], (LAYERS, D, DC), D ** -0.5, 0.125, ((1, 32), (2, 4))),
        "w_c": centred(key_of[4], (LAYERS, D, DC), D ** -0.5, 0.125, ((1, 32), (2, 4))),
        "w_x": centred(key_of[5], (LAYERS, D, DC), D ** -0.5, 0.125, ((1, 32), (2, 4))),
        "taps": centred(key_of[6], (LAYERS, KERNEL, DC), KERNEL ** -0.5, 3.5, (), jnp.float32),
        "w_out": centred(key_of[7], (LAYERS, DC, D), DC ** -0.5, 0.25, ((1, 4), (2, 32))),
    }


epsilon = 1e-06

def normed(activations, gain_row):
    values_f = activations.astype(jnp.float32)
    scale = lax.rsqrt(lax.optimization_barrier(jnp.mean(values_f * values_f, axis=-1, keepdims=True)) + epsilon)
    return values_f * scale * gain_row

def reference(tokens, gain_pre, gain_post, w_b, w_c, w_x, taps, w_out):
    stream = tokens
    for layer_index in range(LAYERS):
        hidden = normed(stream, gain_pre[layer_index]).astype(jnp.bfloat16)
        gate_b = jnp.dot(hidden, w_b[layer_index], preferred_element_type=jnp.float32).astype(jnp.bfloat16)
        gate_c = jnp.dot(hidden, w_c[layer_index], preferred_element_type=jnp.float32).astype(jnp.bfloat16)
        values = jnp.dot(hidden, w_x[layer_index], preferred_element_type=jnp.float32).astype(jnp.bfloat16)
        product = (gate_c.astype(jnp.float32) * values.astype(jnp.float32)).astype(jnp.bfloat16)
        padded = jnp.pad(product.astype(jnp.float32), ((KERNEL - 1, 0), (0, 0)))
        row_total = padded.shape[0] - KERNEL + 1
        convolved = jnp.zeros((row_total, DC), jnp.float32)
        for offset in range(KERNEL):
            convolved = convolved + taps[layer_index, offset][None, :] * padded[offset:offset + row_total]
        weighted = (gate_b.astype(jnp.float32) * convolved).astype(jnp.bfloat16)
        branch = jnp.dot(weighted, w_out[layer_index], preferred_element_type=jnp.float32)
        stream = (stream.astype(jnp.float32) + normed(branch, gain_post[layer_index])).astype(jnp.bfloat16)
    return stream
```

```python
import jax
import jax.numpy as jnp
from jax import lax
from jax.experimental import pallas as pl
from jax.experimental.pallas import tpu as pltpu
from jax.sharding import PartitionSpec as P

epsilon = 1e-06
HALO = 32
TILES = 2
MATS = 4


def rms(values_f):
    return lax.rsqrt(jnp.mean(values_f * values_f, axis=-1, keepdims=True) + epsilon)


def nt_dot(a, b):
    return lax.dot_general(a, b, (((1,), (1,)), ((), ())), preferred_element_type=jnp.float32)


def layer_body(stream, weights, gain_pre, taps, gain_post, conv_ref, branch_ref):
    rows = stream.shape[0]
    kernel_size = taps.shape[0]
    values_f = stream.astype(jnp.float32)
    hidden = (values_f * rms(values_f) * gain_pre).astype(jnp.bfloat16)
    project = lambda m: jnp.dot(hidden, weights(m), preferred_element_type=jnp.float32).astype(jnp.bfloat16)
    gate_c = project(1)
    values = project(2)
    product = (gate_c.astype(jnp.float32) * values.astype(jnp.float32)).astype(jnp.bfloat16)
    conv_ref[pl.ds(8, rows), :] = product.astype(jnp.float32)
    convolved = taps[0:1] * conv_ref[pl.ds(8 - kernel_size + 1, rows), :]
    for k in range(1, kernel_size):
        convolved = convolved + taps[k : k + 1] * conv_ref[pl.ds(8 - kernel_size + 1 + k, rows), :]
    gate_b = project(0)
    weighted = (gate_b.astype(jnp.float32) * convolved).astype(jnp.bfloat16)
    conv_ref[0:8, :] = conv_ref[pl.ds(rows, 8), :]
    branch_ref[...] = nt_dot(weighted, weights(3))
    branch = branch_ref[...]
    return (stream.astype(jnp.float32) + branch * rms(branch) * gain_post).astype(jnp.bfloat16)


def mixer(copies, sources, gain_pre, taps, gain_post, stream_parts, dims, out_rows, name):
    d, dc, sp, block_rows = dims
    total = sum(p.shape[0] for p in stream_parts)
    tile = total // TILES
    skip = total - out_rows
    n_src, n_parts = len(sources), len(stream_parts)

    def kernel(*refs):
        src = refs[:n_src]
        parts = refs[n_src : n_src + n_parts]
        pre_ref, taps_ref, post_ref, out_ref = refs[n_src + n_parts : n_src + n_parts + 4]
        w_ref, x_ref, conv_ref, branch_ref, res_ref, w_sem, x_sem, o_sem = refs[n_src + n_parts + 4 :]

        def part_copies():
            start = 0
            for k, p in enumerate(parts):
                yield pltpu.make_async_copy(p, x_ref.at[pl.ds(start, p.shape[0])], x_sem.at[k])
                start += p.shape[0]

        for c in part_copies():
            c.start()
        for s, t in copies(src, w_ref):
            pltpu.make_async_copy(s, t, w_sem).start()
        conv_ref[0:8, :] = jnp.zeros((8, dc), jnp.float32)
        for c in part_copies():
            c.wait()
        for s, t in copies(src, w_ref):
            pltpu.make_async_copy(s, t, w_sem).wait()

        def out_copy(i):
            first = skip if i == 0 else 0
            n = tile - first
            return pltpu.make_async_copy(
                res_ref.at[i, pl.ds(first, n)], out_ref.at[pl.ds(i * tile - skip + first, n)], o_sem.at[i]
            )

        def step(i, carry):
            row = pl.multiple_of(i * tile, 16)
            res_ref[i] = layer_body(
                x_ref[pl.ds(row, tile), :],
                lambda m: w_ref[m].reshape(d, dc),
                pre_ref[...],
                taps_ref[...],
                post_ref[...],
                conv_ref,
                branch_ref,
            )
            return carry

        lax.fori_loop(0, TILES, step, 0)
        for i in range(TILES):
            out_copy(i).start()
        for i in range(TILES):
            out_copy(i).wait()

    hbm = pl.BlockSpec(memory_space=pltpu.MemorySpace.HBM)
    vmem = pl.BlockSpec(memory_space=pltpu.MemorySpace.VMEM)
    return pl.pallas_call(
        kernel,
        out_shape=jax.ShapeDtypeStruct((out_rows, d), jnp.bfloat16),
        in_specs=[hbm] * (n_src + n_parts) + [vmem] * 3,
        out_specs=hbm,
        scratch_shapes=[
            pltpu.VMEM((MATS, sp, block_rows, dc), jnp.bfloat16),
            pltpu.VMEM((total, d), jnp.bfloat16),
            pltpu.VMEM((tile + 8, dc), jnp.float32),
            pltpu.VMEM((tile, d), jnp.float32),
            pltpu.VMEM((TILES, tile, d), jnp.bfloat16),
            pltpu.SemaphoreType.DMA,
            pltpu.SemaphoreType.DMA((n_parts,)),
            pltpu.SemaphoreType.DMA((TILES,)),
        ],
        compiler_params=pltpu.CompilerParams(vmem_limit_bytes=56 * 2**20),
        name=name,
    )(*sources, *stream_parts, gain_pre, taps, gain_post)


def turned(axis, size, stride, distance):
    n = size // stride
    return [(((i // stride + distance) % n) * stride + i % stride, i) for i in range(size)]


def receive(value, axis, distance, stride=1):
    return lax.ppermute(value, axis, turned(axis, lax.axis_size(axis), stride, distance))


def other_core(value):
    return lax.ppermute(value, "sp", [(i ^ 1, i) for i in range(lax.axis_size("sp"))])


def early_halo(tokens):
    axes = ("sp", "tp")
    total = lax.axis_size(axes)
    return lax.ppermute(tokens[-HALO:], axes, [(i - 1, i) for i in range(1, total)])


def on_device(tokens, gain_pre, gain_post, w_b, w_c, w_x, taps, w_out):
    layer_total, block_rows, block_cols = w_b.shape
    sp, tp = lax.axis_size("sp"), lax.axis_size("tp")
    d, dc = sp * block_rows, tp * block_cols
    dims = (d, dc, sp, block_rows)
    chips = sp // 2
    own = [
        jnp.stack([w_b[l], w_c[l], w_x[l], w_out[l].T]) for l in range(layer_total)
    ]

    last = own[1]
    along = jnp.stack([last] + [receive(last, "tp", k) for k in range(1, tp)])
    gathered = lax.all_gather(along, "sp", axis=0)
    halo = early_halo(tokens)

    z = lambda value, distance: receive(value, "sp", distance, 2)
    quarter = chips // 4
    first = own[0]
    one = jnp.stack([first, z(first, quarter), z(first, 2 * quarter), z(first, -quarter)])
    wrap = jnp.stack([one[3], one[0]])
    two = jnp.concatenate([one, z(one, 1), z(one[:2], 2), z(wrap, -2), z(one, -1)])
    offsets = (
        [quarter * k for k in range(4)]
        + [1 + quarter * k for k in range(4)]
        + [2, 2 + quarter]
        + [-2 + 3 * quarter, -2]
        + [-1 + quarter * k for k in range(4)]
    )
    half = chips // 2
    ahead = receive(two, "tp", 1)
    behind = receive(two, "tp", -1)
    far_a = receive(ahead[:half], "tp", 1)
    far_b = receive(behind[half:], "tp", -1)
    mine = [two, ahead, behind, far_a, far_b]
    theirs = [other_core(value) for value in mine]
    places = [(0, 0), (1, 0), (-1, 0), (2, 0), (2, half)]

    def first_copies(src, w_ref):
        here_sp, here_tp = lax.axis_index("sp"), lax.axis_index("tp")
        chip, core = here_sp // 2, here_sp % 2
        for side in range(2):
            side_core = core if side == 0 else 1 - core
            for p, (column, begin) in enumerate(places):
                ref = src[side * len(places) + p]
                lanes = pl.multiple_of(((here_tp + column + tp) % tp) * block_cols, block_cols)
                for k in range(ref.shape[0]):
                    row = ((chip + offsets[begin + k] + chips) % chips) * 2 + side_core
                    yield ref.at[k], w_ref.at[:, row, :, pl.ds(lanes, block_cols)]

    def last_copies(src, w_ref):
        here_tp = lax.axis_index("tp")
        for k in range(tp):
            lanes = pl.multiple_of(((here_tp + k) % tp) * block_cols, block_cols)
            for m in range(MATS):
                yield src[0].at[:, k, m], w_ref.at[m, :, :, pl.ds(lanes, block_cols)]

    row_of = lambda a, l: a[l][None, :]
    rows = tokens.shape[0]
    stream = mixer(
        first_copies, mine + theirs, row_of(gain_pre, 0), taps[0], row_of(gain_post, 0),
        [halo, tokens], dims, rows + HALO, "mixer_first",
    )
    return mixer(
        last_copies, [gathered], row_of(gain_pre, 1), taps[1], row_of(gain_post, 1),
        [stream], dims, rows, "mixer_last",
    )


def solution(mesh):
    placed = (
        P(("grp", "sp", "tp"), None),
        P(),
        P(),
        P(None, "sp", "tp"),
        P(None, "sp", "tp"),
        P(None, "sp", "tp"),
        P(),
        P(None, "tp", "sp"),
    )
    return jax.shard_map(
        on_device,
        mesh=mesh,
        in_specs=placed,
        out_specs=P(("grp", "sp", "tp"), None),
        check_vma=False,
    )
```

```python
import jax
import jax.numpy as jnp
from jax import lax
from jax.experimental import pallas as pl
from jax.experimental.pallas import tpu as pltpu
from jax.sharding import PartitionSpec as P


epsilon = 1e-06
HALO = 32
TILES = 2
MATS = 4
MAT_ORDER = (1, 2, 0, 3)


def rms(values_f):
    return lax.rsqrt(jnp.mean(values_f * values_f, axis=-1, keepdims=True) + epsilon)


def nt_dot(a, b):
    return lax.dot_general(a, b, (((1,), (1,)), ((), ())), preferred_element_type=jnp.float32)


def normed(values_f, gain):
    return values_f * rms(values_f) * gain


def layer_body(stream, hidden, weights, taps, gain_post, conv_ref, branch_ref):
    rows = stream.shape[0]
    kernel_size = taps.shape[0]
    project = lambda m: jnp.dot(hidden, weights(m), preferred_element_type=jnp.float32).astype(jnp.bfloat16)
    gate_c = project(1)
    values = project(2)
    product = (gate_c.astype(jnp.float32) * values.astype(jnp.float32)).astype(jnp.bfloat16)
    conv_ref[pl.ds(8, rows), :] = product.astype(jnp.float32)
    convolved = taps[0:1] * conv_ref[pl.ds(8 - kernel_size + 1, rows), :]
    for k in range(1, kernel_size):
        convolved = convolved + taps[k : k + 1] * conv_ref[pl.ds(8 - kernel_size + 1 + k, rows), :]
    gate_b = project(0)
    weighted = (gate_b.astype(jnp.float32) * convolved).astype(jnp.bfloat16)
    conv_ref[0:8, :] = conv_ref[pl.ds(rows, 8), :]
    branch_ref[...] = nt_dot(weighted, weights(3))
    return (stream.astype(jnp.float32) + normed(branch_ref[...], gain_post)).astype(jnp.bfloat16)


def mixer(copies, groups, sources, gain_pre, taps, gain_post, stream_parts, dims, out_rows):
    d, dc, sp, block_rows = dims
    total = sum(p.shape[0] for p in stream_parts)
    tile = total // TILES
    skip = total - out_rows
    n_src, n_parts = len(sources), len(stream_parts)

    def kernel(*refs):
        src = refs[:n_src]
        parts = refs[n_src : n_src + n_parts]
        pre_ref, taps_ref, post_ref, out_ref = refs[n_src + n_parts : n_src + n_parts + 4]
        w_ref, x_ref, h_ref, conv_ref, branch_ref, res_ref, w_sem, x_sem, o_sem = refs[n_src + n_parts + 4 :]

        def part_copies():
            start = 0
            for k, p in enumerate(parts):
                yield pltpu.make_async_copy(p, x_ref.at[pl.ds(start, p.shape[0])], x_sem.at[k])
                start += p.shape[0]

        for c in part_copies():
            c.start()
        copies(src, w_ref, w_sem)
        conv_ref[0:8, :] = jnp.zeros((8, dc), jnp.float32)
        for c in part_copies():
            c.wait()

        def rows_of(i):
            return pl.ds(pl.multiple_of(i * tile, 16), tile)

        def norm_step(i, carry):
            h_ref[rows_of(i), :] = normed(x_ref[rows_of(i), :].astype(jnp.float32), pre_ref[...]).astype(jnp.bfloat16)
            return carry

        lax.fori_loop(0, TILES, norm_step, 0)

        def arrive(i, m):
            if groups == 1 and m == MAT_ORDER[0]:
                pl.when(i == 0)(lambda: pltpu.make_async_copy(w_ref, w_ref, w_sem.at[0]).wait())
            if groups > 1:
                copy = pltpu.make_async_copy(w_ref.at[m], w_ref.at[m], w_sem.at[MAT_ORDER.index(m)])
                pl.when(i == 0)(lambda: copy.wait())

        def out_copy(i):
            first = skip if i == 0 else 0
            n = tile - first
            return pltpu.make_async_copy(
                res_ref.at[i, pl.ds(first, n)], out_ref.at[pl.ds(i * tile - skip + first, n)], o_sem.at[i]
            )

        def step(i, carry):
            def weights(m):
                arrive(i, m)
                return w_ref[m].reshape(d, dc)

            res_ref[i] = layer_body(
                x_ref[rows_of(i), :],
                h_ref[rows_of(i), :],
                weights,
                taps_ref[...],
                post_ref[...],
                conv_ref,
                branch_ref,
            )
            for k in range(TILES):
                pl.when(i == k)(lambda k=k: out_copy(k).start())
            return carry

        lax.fori_loop(0, TILES, step, 0)
        for i in range(TILES):
            out_copy(i).wait()

    hbm = pl.BlockSpec(memory_space=pltpu.MemorySpace.HBM)
    vmem = pl.BlockSpec(memory_space=pltpu.MemorySpace.VMEM)
    return pl.pallas_call(
        kernel,
        out_shape=jax.ShapeDtypeStruct((out_rows, d), jnp.bfloat16),
        in_specs=[hbm] * (n_src + n_parts) + [vmem] * 3,
        out_specs=hbm,
        scratch_shapes=[
            pltpu.VMEM((MATS, sp, block_rows, dc), jnp.bfloat16),
            pltpu.VMEM((total, d), jnp.bfloat16),
            pltpu.VMEM((total, d), jnp.bfloat16),
            pltpu.VMEM((tile + 8, dc), jnp.float32),
            pltpu.VMEM((tile, d), jnp.float32),
            pltpu.VMEM((TILES, tile, d), jnp.bfloat16),
            pltpu.SemaphoreType.DMA((groups,)),
            pltpu.SemaphoreType.DMA((n_parts,)),
            pltpu.SemaphoreType.DMA((TILES,)),
        ],
        cost_estimate=pl.CostEstimate(
            flops=2 * MATS * total * d * dc, transcendentals=0, bytes_accessed=2 * (MATS * d * dc + 2 * total * d)
        ),
        compiler_params=pltpu.CompilerParams(vmem_limit_bytes=56 * 2**20),
    )(*sources, *stream_parts, gain_pre, taps, gain_post)


def turned(size, stride, distance):
    n = size // stride
    return [(((i // stride + distance) % n) * stride + i % stride, i) for i in range(size)]


def receive(value, axis, distance, stride=1):
    return lax.ppermute(value, axis, turned(lax.axis_size(axis), stride, distance))


def other_core(value):
    return lax.ppermute(value, "sp", [(i ^ 1, i) for i in range(lax.axis_size("sp"))])


def early_halo(tokens):
    axes = ("sp", "tp")
    total = lax.axis_size(axes)
    return lax.ppermute(tokens[-HALO:], axes, [(i - 1, i) for i in range(1, total)])


def on_device(tokens, gain_pre, gain_post, w_b, w_c, w_x, taps, w_out):
    layer_total, block_rows, block_cols = w_b.shape
    sp, tp = lax.axis_size("sp"), lax.axis_size("tp")
    d, dc = sp * block_rows, tp * block_cols
    dims = (d, dc, sp, block_rows)
    chips = sp // 2
    half = chips // 2
    quarter = chips // 4
    z = lambda value, distance: receive(value, "sp", distance, 2)
    x = lambda value, distance: receive(value, "tp", distance)
    own = [jnp.stack([w_b[l], w_c[l], w_x[l], w_out[l].T]) for l in range(layer_total)]

    share = MATS // 2
    places = [(0, 0), (1, 0), (-1, 0), (2, 0), (2, half)]

    along = jnp.stack([own[1]] + [x(own[1], k) for k in range(1, tp)])
    gathered = lax.all_gather(along, "sp", axis=0)
    part = lax.dynamic_slice_in_dim(own[0], share * (lax.axis_index("grp") % 2), share)
    one = jnp.stack([part, z(part, quarter), z(part, 2 * quarter), z(part, -quarter)])
    wrap = jnp.stack([one[3], one[0]])
    kept = jnp.concatenate([one, z(one, 1), z(one[:2], 2), z(wrap, -2), z(one, -1)])

    def along_tp(two):
        ahead = x(two, 1)
        behind = x(two, -1)
        theirs = [other_core(two)]
        far_a = x(ahead[:half], 1)
        far_b = x(behind[half:], -1)
        mine = [two, ahead, behind, far_a, far_b]
        theirs += [other_core(value) for value in mine[1:]]
        return mine + theirs

    other = lax.ppermute(kept, "grp", [(i ^ 1, i) for i in range(lax.axis_size("grp"))])
    halo = early_halo(tokens)
    pieces = along_tp(kept) + along_tp(other)

    def first_copies(src, w_ref, w_sem):
        here_sp, here_tp, parity = lax.axis_index("sp"), lax.axis_index("tp"), lax.axis_index("grp") % 2
        chip, core = here_sp // 2, here_sp % 2
        for n, ref in enumerate(src):
            second, side, p = n // (2 * len(places)), n // len(places) % 2, n % len(places)
            column, begin = places[p]
            mats = pl.ds(share * (parity if second == 0 else 1 - parity), share)
            side_core = core if side == 0 else 1 - core
            lanes = pl.multiple_of(((here_tp + column + tp) % tp) * block_cols, block_cols)

            def start(k, carry):
                place = begin + k
                step = place // 4
                offset = quarter * (place % 4) + jnp.where(step == 3, -1, step)
                row = ((chip + offset + chips) % chips) * 2 + side_core
                target = w_ref.at[mats, row, :, pl.ds(lanes, block_cols)]
                pltpu.make_async_copy(ref.at[k], target, w_sem.at[0]).start()
                return carry

            lax.fori_loop(0, ref.shape[0], start, 0)

    def last_copies(src, w_ref, w_sem):
        here_tp = lax.axis_index("tp")
        for group, m in enumerate(MAT_ORDER):
            for k in range(tp):
                lanes = pl.multiple_of(((here_tp + k) % tp) * block_cols, block_cols)
                target = w_ref.at[m, :, :, pl.ds(lanes, block_cols)]
                pltpu.make_async_copy(src[0].at[:, k, m], target, w_sem.at[group]).start()

    row_of = lambda a, l: a[l][None, :]
    rows = tokens.shape[0]
    stream = mixer(
        first_copies, 1, pieces, row_of(gain_pre, 0), taps[0], row_of(gain_post, 0),
        [halo, tokens], dims, rows + HALO,
    )
    return mixer(
        last_copies, MATS, [gathered], row_of(gain_pre, 1), taps[1], row_of(gain_post, 1),
        [stream], dims, rows,
    )


def solution(mesh):
    placed = (
        P(("grp", "sp", "tp"), None),
        P(),
        P(),
        P(None, "sp", "tp"),
        P(None, "sp", "tp"),
        P(None, "sp", "tp"),
        P(),
        P(None, "tp", "sp"),
    )
    return jax.shard_map(
        on_device,
        mesh=mesh,
        in_specs=placed,
        out_specs=P(("grp", "sp", "tp"), None),
        check_vma=False,
    )
```

```python
import jax
import jax.numpy as jnp
from jax import lax
from jax.experimental import pallas as pl
from jax.experimental.pallas import tpu as pltpu
from jax.sharding import PartitionSpec as P


epsilon = 1e-06
HALO = 32
CHUNKS = 2
BANDS = 1
MATS = 4


def rms(values_f):
    return lax.rsqrt(jnp.mean(values_f * values_f, axis=-1, keepdims=True) + epsilon)


def nt_dot(a, b):
    return lax.dot_general(a, b, (((1,), (1,)), ((), ())), preferred_element_type=jnp.float32)


def normed(values_f, gain):
    return values_f * rms(values_f) * gain


def normed(values_f, gain):
    return values_f * rms(values_f) * gain


def chunks_of(total):
    size = total // CHUNKS
    return [slice(k * size, (k + 1) * size) for k in range(CHUNKS)]


HBM = pl.BlockSpec(memory_space=pltpu.MemorySpace.HBM)
VMEM = pl.BlockSpec(memory_space=pltpu.MemorySpace.VMEM)


def end_to_end(parts, target, sems):
    start = 0
    for k, p in enumerate(parts):
        yield pltpu.make_async_copy(p, target.at[pl.ds(start, p.shape[0])], sems.at[k])
        start += p.shape[0]


def normed_rows(parts, gain):
    total, d = sum(p.shape[0] for p in parts), parts[0].shape[1]
    n = len(parts)

    def kernel(*refs):
        gain_ref, out_ref, x_ref, h_ref, in_sem, out_sem = refs[n:]
        for c in end_to_end(refs[:n], x_ref, in_sem):
            c.start()
        for c in end_to_end(refs[:n], x_ref, in_sem):
            c.wait()
        stores = []
        for k, rows in enumerate(chunks_of(total)):
            h_ref[rows, :] = normed(x_ref[rows, :].astype(jnp.float32), gain_ref[...]).astype(jnp.bfloat16)
            span = pl.ds(rows.start, rows.stop - rows.start)
            stores.append(pltpu.make_async_copy(h_ref.at[span], out_ref.at[span], out_sem.at[k]))
            stores[-1].start()
        for c in stores:
            c.wait()

    return pl.pallas_call(
        kernel,
        out_shape=jax.ShapeDtypeStruct((total, d), jnp.bfloat16),
        in_specs=[HBM] * n + [VMEM],
        out_specs=HBM,
        scratch_shapes=[
            pltpu.VMEM((total, d), jnp.bfloat16),
            pltpu.VMEM((total, d), jnp.bfloat16),
            pltpu.SemaphoreType.DMA((n,)),
            pltpu.SemaphoreType.DMA((CHUNKS,)),
        ],
        cost_estimate=pl.CostEstimate(flops=8 * total * d, transcendentals=0, bytes_accessed=4 * total * d),
        compiler_params=pltpu.CompilerParams(vmem_limit_bytes=40 * 2**20),
    )(*parts, gain)


def two_mixers(copies, sources, hidden, parts, gain_pre, taps, gain_post, dims, out_rows):
    d, dc, sp, block_rows = dims
    total = hidden.shape[0]
    skip = total - out_rows
    pairs, wide = 2, dc // 2
    kernel_size = taps.shape[1]
    counts = [len(group) for group in sources]
    n_src, n_parts = sum(counts), len(parts)

    def kernel(*refs):
        src = [refs[: counts[0]], refs[counts[0] : n_src]]
        part_refs = refs[n_src : n_src + n_parts]
        hidden_ref, pre_ref, taps_ref, post_ref, out_ref = refs[n_src + n_parts : n_src + n_parts + 5]
        w_ref, x_ref, h_ref, c_ref, conv_ref, w_sem, x_sem, o_sem = refs[n_src + n_parts + 5 :]

        copies[0](src[0], w_ref.at[0], w_sem.at[0])
        for c in end_to_end(part_refs, x_ref, x_sem):
            c.start()
        copies[1](src[1], w_ref.at[1], w_sem.at[1])
        conv_ref[0:8, :] = jnp.zeros((8, dc), jnp.float32)
        chunks = chunks_of(total)
        chunk, band = total // CHUNKS, total // BANDS
        h_ref[...] = hidden_ref[...]

        def out_copy(r):
            first = max(chunks[r].start, skip)
            n = chunks[r].stop - first
            return pltpu.make_async_copy(x_ref.at[pl.ds(first, n)], out_ref.at[pl.ds(first - skip, n)], o_sem.at[r])

        def layer(l, carry):
            def pair_step(pair, carry):
                pltpu.make_async_copy(w_ref.at[l, pair], w_ref.at[l, pair], w_sem.at[l, pair]).wait()
                cols = pl.ds(pl.multiple_of(pair * wide, wide), wide)
                tap = lambda k: taps_ref[l, k : k + 1, cols]
                first = 8 - kernel_size + 1

                def band_step(i, carry):
                    start = pl.multiple_of(i * band, 16)

                    def project(m):
                        return jnp.dot(
                            h_ref[pl.ds(start, band), :], w_ref[l, pair, m].reshape(d, wide),
                            preferred_element_type=jnp.float32,
                        ).astype(jnp.bfloat16)

                    gate_c = project(1)
                    product = (gate_c.astype(jnp.float32) * project(2).astype(jnp.float32)).astype(jnp.bfloat16)
                    conv_ref[pl.ds(start + 8, band), cols] = product.astype(jnp.float32)
                    window = conv_ref[pl.ds(start, band + 8), cols]
                    convolved = tap(0) * window[first : first + band]
                    for k in range(1, kernel_size):
                        convolved = convolved + tap(k) * window[first + k : first + k + band]
                    c_ref[pl.ds(start, band), cols] = (project(0).astype(jnp.float32) * convolved).astype(jnp.bfloat16)
                    return carry

                return lax.fori_loop(0, BANDS, band_step, carry)

            lax.fori_loop(0, pairs, pair_step, 0)

            @pl.when(l == 0)
            def _():
                for c in end_to_end(part_refs, x_ref, x_sem):
                    c.wait()

            next_gain = pre_ref[pl.ds(jnp.minimum(l + 1, 1), 1), :]

            def chunk_step(r, carry):
                rows = pl.ds(pl.multiple_of(r * chunk, 16), chunk)
                back = jnp.concatenate([w_ref[l, p, 3].reshape(d, wide) for p in range(pairs)], axis=1)
                branch = nt_dot(c_ref[rows, :], back)
                stream = x_ref[rows, :].astype(jnp.float32) + normed(branch, post_ref[pl.ds(l, 1), :])
                rounded = stream.astype(jnp.bfloat16)
                x_ref[rows, :] = rounded
                h_ref[rows, :] = normed(rounded.astype(jnp.float32), next_gain).astype(jnp.bfloat16)
                for k in range(CHUNKS):
                    pl.when((l == 1) & (r == k))(lambda k=k: out_copy(k).start())
                return carry

            return lax.fori_loop(0, CHUNKS, chunk_step, carry)

        lax.fori_loop(0, 2, layer, 0)
        for r in range(CHUNKS):
            out_copy(r).wait()

    return pl.pallas_call(
        kernel,
        out_shape=jax.ShapeDtypeStruct((out_rows, d), jnp.bfloat16),
        in_specs=[HBM] * (n_src + n_parts) + [VMEM] * 4,
        out_specs=HBM,
        scratch_shapes=[
            pltpu.VMEM((2, pairs, MATS, sp, block_rows, wide), jnp.bfloat16),
            pltpu.VMEM((total, d), jnp.bfloat16),
            pltpu.VMEM((total, d), jnp.bfloat16),
            pltpu.VMEM((total, dc), jnp.bfloat16),
            pltpu.VMEM((total + 8, dc), jnp.float32),
            pltpu.SemaphoreType.DMA((2, pairs)),
            pltpu.SemaphoreType.DMA((n_parts,)),
            pltpu.SemaphoreType.DMA((CHUNKS,)),
        ],
        cost_estimate=pl.CostEstimate(
            flops=4 * MATS * total * d * dc, transcendentals=0, bytes_accessed=4 * MATS * d * dc + 6 * total * d
        ),
        compiler_params=pltpu.CompilerParams(vmem_limit_bytes=56 * 2**20),
    )(*sources[0], *sources[1], *parts, hidden, gain_pre, taps, gain_post)


def turned(size, stride, distance):
    n = size // stride
    return [(((i // stride + distance) % n) * stride + i % stride, i) for i in range(size)]


def receive(value, axis, distance, stride=1):
    return lax.ppermute(value, axis, turned(lax.axis_size(axis), stride, distance))


def other_core(value):
    return lax.ppermute(value, "sp", [(i ^ 1, i) for i in range(lax.axis_size("sp"))])


def early_halo(tokens):
    axes = ("sp", "tp")
    total = lax.axis_size(axes)
    return lax.ppermute(tokens[-HALO:], axes, [(i - 1, i) for i in range(1, total)])


def on_device(tokens, gain_pre, gain_post, w_b, w_c, w_x, taps, w_out):
    layer_total, block_rows, block_cols = w_b.shape
    sp, tp = lax.axis_size("sp"), lax.axis_size("tp")
    d, dc = sp * block_rows, tp * block_cols
    dims = (d, dc, sp, block_rows)
    chips = sp // 2
    half = chips // 2
    quarter = chips // 4
    z = lambda value, distance: receive(value, "sp", distance, 2)
    x = lambda value, distance: receive(value, "tp", distance)
    own = [jnp.stack([w_b[l], w_c[l], w_x[l], w_out[l].T]) for l in range(layer_total)]

    share = MATS // 2
    places = [(0, 0), (1, 0), (-1, 0), (2, 0), (2, half)]

    along = jnp.stack([own[1]] + [x(own[1], k) for k in range(1, tp)])
    gathered = lax.all_gather(along, "sp", axis=0)
    part = lax.dynamic_slice_in_dim(own[0], share * (lax.axis_index("grp") % 2), share)
    one = jnp.stack([part, z(part, quarter), z(part, 2 * quarter), z(part, -quarter)])
    wrap = jnp.stack([one[3], one[0]])
    kept = jnp.concatenate([one, z(one, 1), z(one[:2], 2), z(wrap, -2), z(one, -1)])

    def along_tp(two):
        ahead = x(two, 1)
        behind = x(two, -1)
        theirs = [other_core(two)]
        far_a = x(ahead[:half], 1)
        far_b = x(behind[half:], -1)
        mine = [two, ahead, behind, far_a, far_b]
        theirs += [other_core(value) for value in mine[1:]]
        return mine + theirs

    other = lax.ppermute(kept, "grp", [(i ^ 1, i) for i in range(lax.axis_size("grp"))])
    halo = early_halo(tokens)
    pieces = along_tp(kept) + along_tp(other)

    columns = ((0, 1, tp - 1, 2), tuple(range(tp)))

    def first_copies(src, w_ref, sems):
        here_sp, parity = lax.axis_index("sp"), lax.axis_index("grp") % 2
        chip, core = here_sp // 2, here_sp % 2

        def put(n):
            ref = src[n]
            second, side, p = n // (2 * len(places)), n // len(places) % 2, n % len(places)
            column, begin = places[p]
            place_of = columns[0].index(column % tp)
            pair, lanes = place_of // 2, pl.ds(place_of % 2 * block_cols, block_cols)
            mats = pl.ds(share * (parity if second == 0 else 1 - parity), share)
            side_core = core if side == 0 else 1 - core

            def start(k, carry):
                place = begin + k
                step = place // 4
                offset = quarter * (place % 4) + jnp.where(step == 3, -1, step)
                row = ((chip + offset + chips) % chips) * 2 + side_core
                target = w_ref.at[pair, mats, row, :, lanes]
                pltpu.make_async_copy(ref.at[k], target, sems.at[pair]).start()
                return carry

            lax.fori_loop(0, ref.shape[0], start, 0)

        for column in columns[0]:
            for n in range(len(src)):
                if places[n % len(places)][0] % tp == column:
                    put(n)

    def last_copies(src, w_ref, sems):
        for k in range(tp):
            for m in range(MATS):
                target = w_ref.at[k // 2, m, :, :, pl.ds(k % 2 * block_cols, block_cols)]
                pltpu.make_async_copy(src[0].at[:, k, m], target, sems.at[k // 2]).start()

    def own_order(rows, order):
        here = lax.axis_index("tp")
        return jnp.concatenate(
            [
                lax.dynamic_slice_in_dim(rows, (here + column) % tp * block_cols, block_cols, 1)
                for column in order
            ],
            axis=1,
        )

    own_taps = jnp.stack([own_order(taps[l], columns[l]) for l in range(layer_total)])
    parts = [halo, tokens]
    hidden = normed_rows(parts, gain_pre[0][None, :])
    return two_mixers(
        [first_copies, last_copies], [pieces, [gathered]], hidden, parts, gain_pre, own_taps, gain_post,
        dims, tokens.shape[0],
    )


def solution(mesh):
    placed = (
        P(("grp", "sp", "tp"), None),
        P(),
        P(),
        P(None, "sp", "tp"),
        P(None, "sp", "tp"),
        P(None, "sp", "tp"),
        P(),
        P(None, "tp", "sp"),
    )
    return jax.shard_map(
        on_device,
        mesh=mesh,
        in_specs=placed,
        out_specs=P(("grp", "sp", "tp"), None),
        check_vma=False,
    )
```

```python
import jax
import jax.numpy as jnp
from jax import lax
from jax.experimental import pallas as pl
from jax.experimental.pallas import tpu as pltpu
from jax.sharding import PartitionSpec as P


epsilon = 1e-06
HALO = 32
CHUNKS = 2
BANDS = 1
MATS = 4


def rms(values_f):
    return lax.rsqrt(jnp.mean(values_f * values_f, axis=-1, keepdims=True) + epsilon)


def nt_dot(a, b):
    return lax.dot_general(a, b, (((1,), (1,)), ((), ())), preferred_element_type=jnp.float32)


def normed(values_f, gain):
    return values_f * rms(values_f) * gain


def normed(values_f, gain):
    return values_f * rms(values_f) * gain


def chunks_of(total):
    size = total // CHUNKS
    return [slice(k * size, (k + 1) * size) for k in range(CHUNKS)]


HBM = pl.BlockSpec(memory_space=pltpu.MemorySpace.HBM)
VMEM = pl.BlockSpec(memory_space=pltpu.MemorySpace.VMEM)


def end_to_end(parts, target, sems):
    start = 0
    for k, p in enumerate(parts):
        yield pltpu.make_async_copy(p, target.at[pl.ds(start, p.shape[0])], sems.at[k])
        start += p.shape[0]


def normed_rows(parts, gain):
    total, d = sum(p.shape[0] for p in parts), parts[0].shape[1]
    n = len(parts)

    def kernel(*refs):
        gain_ref, out_ref, x_ref, h_ref, in_sem, out_sem = refs[n:]
        for c in end_to_end(refs[:n], x_ref, in_sem):
            c.start()
        for c in end_to_end(refs[:n], x_ref, in_sem):
            c.wait()
        stores = []
        for k, rows in enumerate(chunks_of(total)):
            h_ref[rows, :] = normed(x_ref[rows, :].astype(jnp.float32), gain_ref[...]).astype(jnp.bfloat16)
            span = pl.ds(rows.start, rows.stop - rows.start)
            stores.append(pltpu.make_async_copy(h_ref.at[span], out_ref.at[span], out_sem.at[k]))
            stores[-1].start()
        for c in stores:
            c.wait()

    return pl.pallas_call(
        kernel,
        out_shape=jax.ShapeDtypeStruct((total, d), jnp.bfloat16),
        in_specs=[HBM] * n + [VMEM],
        out_specs=HBM,
        scratch_shapes=[
            pltpu.VMEM((total, d), jnp.bfloat16),
            pltpu.VMEM((total, d), jnp.bfloat16),
            pltpu.SemaphoreType.DMA((n,)),
            pltpu.SemaphoreType.DMA((CHUNKS,)),
        ],
        cost_estimate=pl.CostEstimate(flops=8 * total * d, transcendentals=0, bytes_accessed=4 * total * d),
        compiler_params=pltpu.CompilerParams(vmem_limit_bytes=40 * 2**20),
    )(*parts, gain)


def two_mixers(copies, sources, hidden, parts, gain_pre, taps, gain_post, dims, out_rows):
    d, dc, sp, block_rows = dims
    total = hidden.shape[0]
    skip = total - out_rows
    pairs, wide = 2, dc // 2
    kernel_size = taps.shape[1]
    counts = [len(group) for group in sources]
    n_src, n_parts = sum(counts), len(parts)

    def kernel(*refs):
        src = [refs[: counts[0]], refs[counts[0] : n_src]]
        part_refs = refs[n_src : n_src + n_parts]
        hidden_ref, pre_ref, taps_ref, post_ref, out_ref = refs[n_src + n_parts : n_src + n_parts + 5]
        w_ref, x_ref, h_ref, c_ref, conv_ref, w_sem, x_sem, o_sem = refs[n_src + n_parts + 5 :]

        copies[0](src[0], w_ref.at[0], w_sem.at[0])
        for c in end_to_end(part_refs, x_ref, x_sem):
            c.start()
        copies[1](src[1], w_ref.at[1], w_sem.at[1])
        conv_ref[0:8, :] = jnp.zeros((8, dc), jnp.float32)
        chunks = chunks_of(total)
        chunk, band = total // CHUNKS, total // BANDS
        h_ref[...] = hidden_ref[...]

        def out_copy(r):
            first = max(chunks[r].start, skip)
            n = chunks[r].stop - first
            return pltpu.make_async_copy(x_ref.at[pl.ds(first, n)], out_ref.at[pl.ds(first - skip, n)], o_sem.at[r])

        def layer(l, carry):
            def pair_step(pair, carry):
                pltpu.make_async_copy(w_ref.at[l, pair], w_ref.at[l, pair], w_sem.at[l, pair]).wait()
                cols = pl.ds(pl.multiple_of(pair * wide, wide), wide)
                tap = lambda k: taps_ref[l, k : k + 1, cols]
                first = 8 - kernel_size + 1

                def band_step(i, carry):
                    start = pl.multiple_of(i * band, 16)

                    def project(m):
                        return jnp.dot(
                            h_ref[pl.ds(start, band), :], w_ref[l, pair, m].reshape(d, wide),
                            preferred_element_type=jnp.float32,
                        ).astype(jnp.bfloat16)

                    gate_c = project(1)
                    product = (gate_c.astype(jnp.float32) * project(2).astype(jnp.float32)).astype(jnp.bfloat16)
                    conv_ref[pl.ds(start + 8, band), cols] = product.astype(jnp.float32)
                    window = conv_ref[pl.ds(start, band + 8), cols]
                    convolved = tap(0) * window[first : first + band]
                    for k in range(1, kernel_size):
                        convolved = convolved + tap(k) * window[first + k : first + k + band]
                    c_ref[pl.ds(start, band), cols] = (project(0).astype(jnp.float32) * convolved).astype(jnp.bfloat16)
                    return carry

                return lax.fori_loop(0, BANDS, band_step, carry)

            lax.fori_loop(0, pairs, pair_step, 0)

            @pl.when(l == 0)
            def _():
                for c in end_to_end(part_refs, x_ref, x_sem):
                    c.wait()

            next_gain = pre_ref[pl.ds(jnp.minimum(l + 1, 1), 1), :]

            def chunk_step(r, carry):
                rows = pl.ds(pl.multiple_of(r * chunk, 16), chunk)
                back = jnp.concatenate([w_ref[l, p, 3].reshape(d, wide) for p in range(pairs)], axis=1)
                branch = nt_dot(c_ref[rows, :], back)
                stream = x_ref[rows, :].astype(jnp.float32) + normed(branch, post_ref[pl.ds(l, 1), :])
                rounded = stream.astype(jnp.bfloat16)
                x_ref[rows, :] = rounded

                @pl.when(l == 0)
                def _():
                    h_ref[rows, :] = normed(rounded.astype(jnp.float32), next_gain).astype(jnp.bfloat16)

                for k in range(CHUNKS):
                    pl.when((l == 1) & (r == k))(lambda k=k: out_copy(k).start())
                return carry

            return lax.fori_loop(0, CHUNKS, chunk_step, carry)

        lax.fori_loop(0, 2, layer, 0)
        for r in range(CHUNKS):
            out_copy(r).wait()

    return pl.pallas_call(
        kernel,
        out_shape=jax.ShapeDtypeStruct((out_rows, d), jnp.bfloat16),
        in_specs=[HBM] * (n_src + n_parts) + [VMEM] * 4,
        out_specs=HBM,
        scratch_shapes=[
            pltpu.VMEM((2, pairs, MATS, sp, block_rows, wide), jnp.bfloat16),
            pltpu.VMEM((total, d), jnp.bfloat16),
            pltpu.VMEM((total, d), jnp.bfloat16),
            pltpu.VMEM((total, dc), jnp.bfloat16),
            pltpu.VMEM((total + 8, dc), jnp.float32),
            pltpu.SemaphoreType.DMA((2, pairs)),
            pltpu.SemaphoreType.DMA((n_parts,)),
            pltpu.SemaphoreType.DMA((CHUNKS,)),
        ],
        cost_estimate=pl.CostEstimate(
            flops=4 * MATS * total * d * dc, transcendentals=0, bytes_accessed=4 * MATS * d * dc + 6 * total * d
        ),
        compiler_params=pltpu.CompilerParams(vmem_limit_bytes=56 * 2**20),
    )(*sources[0], *sources[1], *parts, hidden, gain_pre, taps, gain_post)


def turned(size, stride, distance):
    n = size // stride
    return [(((i // stride + distance) % n) * stride + i % stride, i) for i in range(size)]


def receive(value, axis, distance, stride=1):
    return lax.ppermute(value, axis, turned(lax.axis_size(axis), stride, distance))


def other_core(value):
    return lax.ppermute(value, "sp", [(i ^ 1, i) for i in range(lax.axis_size("sp"))])


def early_halo(tokens):
    axes = ("sp", "tp")
    total = lax.axis_size(axes)
    return lax.ppermute(tokens[-HALO:], axes, [(i - 1, i) for i in range(1, total)])


def on_device(tokens, gain_pre, gain_post, w_b, w_c, w_x, taps, w_out):
    layer_total, block_rows, block_cols = w_b.shape
    sp, tp = lax.axis_size("sp"), lax.axis_size("tp")
    d, dc = sp * block_rows, tp * block_cols
    dims = (d, dc, sp, block_rows)
    chips = sp // 2
    half = chips // 2
    quarter = chips // 4
    z = lambda value, distance: receive(value, "sp", distance, 2)
    x = lambda value, distance: receive(value, "tp", distance)
    own = [jnp.stack([w_b[l], w_c[l], w_x[l], w_out[l].T]) for l in range(layer_total)]

    share = MATS // 2
    places = [(0, 0), (1, 0), (-1, 0), (2, 0), (2, half)]

    along = jnp.stack([own[1]] + [x(own[1], k) for k in range(1, tp)])
    gathered = lax.all_gather(along, "sp", axis=0)
    part = lax.dynamic_slice_in_dim(own[0], share * (lax.axis_index("grp") % 2), share)
    one = jnp.stack([part, z(part, quarter), z(part, 2 * quarter), z(part, -quarter)])
    wrap = jnp.stack([one[3], one[0]])
    kept = jnp.concatenate([one, z(one, 1), z(one[:2], 2), z(wrap, -2), z(one, -1)])

    def along_tp(two):
        ahead = x(two, 1)
        behind = x(two, -1)
        theirs = [other_core(two)]
        far_a = x(ahead[:half], 1)
        far_b = x(behind[half:], -1)
        mine = [two, ahead, behind, far_a, far_b]
        theirs += [other_core(value) for value in mine[1:]]
        return mine + theirs

    other = lax.ppermute(kept, "grp", [(i ^ 1, i) for i in range(lax.axis_size("grp"))])
    halo = early_halo(tokens)
    pieces = along_tp(kept) + along_tp(other)

    columns = ((0, 1, tp - 1, 2), tuple(range(tp)))

    def first_copies(src, w_ref, sems):
        here_sp, parity = lax.axis_index("sp"), lax.axis_index("grp") % 2
        chip, core = here_sp // 2, here_sp % 2

        places_along = [(quarter * (place % 4) + (0, 1, 2, -1)[place // 4]) % chips for place in range(chips)]
        row_of = [[(chip + away) % chips * 2 + c for away in places_along] for c in (core, 1 - core)]
        mats_of = [pl.ds(share * parity, share), pl.ds(share * (1 - parity), share)]

        def put(n):
            second, side, p = n // (2 * len(places)), n // len(places) % 2, n % len(places)
            column, begin = places[p]
            place_of = columns[0].index(column % tp)
            pair, lanes = place_of // 2, pl.ds(place_of % 2 * block_cols, block_cols)
            for k in range(src[n].shape[0]):
                target = w_ref.at[pair, mats_of[second], row_of[side][begin + k], :, lanes]
                pltpu.make_async_copy(src[n].at[k], target, sems.at[pair]).start()

        for column in columns[0]:
            for n in range(len(src)):
                if places[n % len(places)][0] % tp == column:
                    put(n)

    def last_copies(src, w_ref, sems):
        for k in range(tp):
            for m in range(MATS):
                target = w_ref.at[k // 2, m, :, :, pl.ds(k % 2 * block_cols, block_cols)]
                pltpu.make_async_copy(src[0].at[:, k, m], target, sems.at[k // 2]).start()

    def own_order(rows, order):
        here = lax.axis_index("tp")
        return jnp.concatenate(
            [
                lax.dynamic_slice_in_dim(rows, (here + column) % tp * block_cols, block_cols, 1)
                for column in order
            ],
            axis=1,
        )

    own_taps = jnp.stack([own_order(taps[l], columns[l]) for l in range(layer_total)])
    parts = [halo, tokens]
    hidden = normed_rows(parts, gain_pre[0][None, :])
    return two_mixers(
        [first_copies, last_copies], [pieces, [gathered]], hidden, parts, gain_pre, own_taps, gain_post,
        dims, tokens.shape[0],
    )


def solution(mesh):
    placed = (
        P(("grp", "sp", "tp"), None),
        P(),
        P(),
        P(None, "sp", "tp"),
        P(None, "sp", "tp"),
        P(None, "sp", "tp"),
        P(),
        P(None, "tp", "sp"),
    )
    return jax.shard_map(
        on_device,
        mesh=mesh,
        in_specs=placed,
        out_specs=P(("grp", "sp", "tp"), None),
        check_vma=False,
    )
```
